128 devices in a mesh: sp: 32 (over z, y, core), tp: 4 (over x).
Axes of the slice: x: 4, y: 4, z: 4, core: 2. Of those that a mesh axis runs over, the one named last changes fastest.
Arguments:
- tokens: bfloat16 [4, 2048, 1024], P(None, 'sp', 'tp'), may hold values from -6 to 6
- norm_gain: float32 [4, 1024], replicated, may hold values from 0.1 to 1.9
- val_weight: bfloat16 [4, 1024, 512], P(None, 'sp', 'tp'), may hold values from -0.1875 to 0.1875
- gate_weight: bfloat16 [4, 1024, 512], P(None, 'sp', 'tp'), may hold values from -0.1875 to 0.1875
- conv_taps: float32 [4, 31, 512], P(None, None, 'tp'), may hold values from -1 to 1
- conv_bias: float32 [4, 512], P(None, 'tp'), may hold values from -3 to 3
- ln_gain: float32 [4, 512], P(None, 'tp'), may hold values from 0.1 to 1.9
- ln_shift: float32 [4, 512], P(None, 'tp'), may hold values from -3 to 3
- out_weight: bfloat16 [4, 512, 1024], P(None, 'tp', 'sp'), may hold values from -0.25 to 0.25
Outputs:
- stream: bfloat16 [4, 2048, 1024], P(None, 'sp', 'tp')
The draws below stay inside these ranges and needn't reach their ends.
All inputs are finite; a program needn't handle non-finite values.
Results may differ from the reference program's by a relative error of at most 0.02.
Values may be sent and summed in bfloat16 or wider, within the bound.
A program may use at most 64 MiB of HBM per device.

```python
import jax
import jax.numpy as jnp
from jax import lax

D = 1024
CHANNELS = 512
TAPS = 31
LAYERS = 4
SEQS = 4
TOKENS = 2048


def level_of(stream_key, dims, shards, low, top_value):
    level = 1.0
    for axis_at, shards_of in shards:
        heights = jax.random.uniform(jax.random.fold_in(jax.random.fold_in(stream_key, 6), axis_at), (shards_of,), jnp.float32, low / len(shards), top_value / len(shards))
        level = level * jnp.repeat(jnp.exp(heights), dims[axis_at] // shards_of).reshape((-1,) + (1,) * (len(dims) - 1 - axis_at))
    return level


def normal_values(own_key, shape, scale, most, shards=(), dtype=jnp.bfloat16):
    result = scale * jax.random.normal(own_key, shape, jnp.float32)
    if shards:
        result = result * level_of(own_key, shape, shards, -0.22, 0.18)
    return jnp.clip(result, -most, most).astype(dtype)


def setup_inputs(seed: int = 0) -> dict:
    splits = jax.random.split(jax.random.key(seed), 10)
    tokens = normal_values(splits[0], (SEQS, TOKENS, D), 1.0, 6.0, ((1, 32), (2, 4)))
    norm_gain = jnp.clip(1.0 + 0.18 * jax.random.normal(splits[1], (LAYERS, D), jnp.float32), 0.1, 1.9)
    val_weight = normal_values(splits[2], (LAYERS, D, CHANNELS), D ** -0.5, 0.1875, ((1, 32), (2, 4)))
    gate_weight = normal_values(splits[3], (LAYERS, D, CHANNELS), D ** -0.5, 0.1875, ((1, 32), (2, 4)))
    conv_taps = normal_values(splits[4], (LAYERS, TAPS, CHANNELS), TAPS ** -0.5, 1.0, ((2, 4),), jnp.float32)
    conv_bias = normal_values(splits[5], (LAYERS, CHANNELS), 0.5, 3.0, ((1, 4),), jnp.float32)
    ln_gain = jnp.clip(1.0 + 0.18 * jax.random.normal(splits[6], (LAYERS, CHANNELS), jnp.float32), 0.1, 1.9)
    ln_shift = normal_values(splits[7], (LAYERS, CHANNELS), 0.5, 3.0, ((1, 4),), jnp.float32)
    out_weight = normal_values(splits[8], (LAYERS, CHANNELS, D), CHANNELS ** -0.5, 0.25, ((1, 4), (2, 32)))
    return {"tokens": tokens, "norm_gain": norm_gain, "val_weight": val_weight, "gate_weight": gate_weight, "conv_taps": conv_taps, "conv_bias": conv_bias, "ln_gain": ln_gain, "ln_shift": ln_shift, "out_weight": out_weight}


epsilon = 1e-06

def depthwise(padded, tap_weights, length):
    running = padded[:, 0:length] * tap_weights[0]
    for tap_idx in range(1, tap_weights.shape[0]):
        running = running + padded[:, tap_idx:tap_idx + length] * tap_weights[tap_idx]
    return running

def reference(tokens, norm_gain, val_weight, gate_weight, conv_taps, conv_bias, ln_gain, ln_shift, out_weight):
    stream = tokens
    half_width = TAPS // 2
    for layer_idx in range(LAYERS):
        widened = stream.astype(jnp.float32)
        scaled = widened * jax.lax.rsqrt(lax.optimization_barrier(jnp.mean(widened * widened, axis=-1, keepdims=True)) + epsilon)
        normed = (scaled * norm_gain[layer_idx]).astype(jnp.bfloat16)
        tok_rows = normed.reshape(-1, D)
        values = jnp.dot(tok_rows, val_weight[layer_idx], preferred_element_type=jnp.float32)
        gates = jnp.dot(tok_rows, gate_weight[layer_idx], preferred_element_type=jnp.float32)
        gated = (values * jax.nn.sigmoid(gates)).astype(jnp.bfloat16).reshape(SEQS, TOKENS, CHANNELS)
        padded = jnp.pad(gated.astype(jnp.float32), ((0, 0), (half_width, half_width), (0, 0)))
        convolved = depthwise(padded, conv_taps[layer_idx], TOKENS) + conv_bias[layer_idx]
        mean_val = lax.optimization_barrier(jnp.mean(convolved, axis=-1, keepdims=True))
        centered = convolved - mean_val
        spread = lax.optimization_barrier(jnp.mean(centered * centered, axis=-1, keepdims=True))
        normalized = centered * jax.lax.rsqrt(spread + epsilon) * ln_gain[layer_idx] + ln_shift[layer_idx]
        activated = jax.nn.silu(normalized).astype(jnp.bfloat16).reshape(-1, CHANNELS)
        branch = jnp.dot(activated, out_weight[layer_idx], preferred_element_type=jnp.float32)
        stream = (stream.astype(jnp.float32) + branch.reshape(SEQS, TOKENS, D)).astype(jnp.bfloat16)
    return stream
```

```python
import functools

import jax
import jax.numpy as jnp
from jax import lax
from jax.experimental import pallas as pl
from jax.experimental.pallas import tpu as pltpu
from jax.sharding import PartitionSpec as P

LAYERS = 4
RING = 4
BLOCK = 64
HALO = 16
FEATS = 256
CHANS = 128
SHARD = 32
TAPS = 31
HALF = 16
EPS = 1e-6
MESH = pl.DeviceIdType.MESH

ORDER = (("x", "y", "z"), ("y", "z", "x"), ("z", "x", "y"))


class Copies:
    def __init__(self, send_sems, recv_sems):
        self.send_sems, self.recv_sems = send_sems, recv_sems
        self.all = []

    def start(self, src, dst, device):
        at = len(self.all)
        copy = pltpu.make_async_remote_copy(
            src_ref=src,
            dst_ref=dst,
            send_sem=self.send_sems.at[at],
            recv_sem=self.recv_sems.at[at],
            device_id=device,
            device_id_type=MESH,
        )
        copy.start()
        self.all.append(copy)
        return copy


def kernel(
    tok_in, gain_in, val_in, gate_in, taps_in, bias_in, lng_in, lns_in, out_in,
    out_ref,
    W, S, taps, chan, gain, gbuf, cbuf, nbuf, abuf, tok, own_taps, obuf,
    local_sems, send_sems, recv_sems,
):
    sp, x = lax.axis_index("sp"), lax.axis_index("tp")
    z, y, c = sp // 8, (sp // 2) % 4, sp % 2
    own = {"x": x, "y": y, "z": z}

    def device(c_=None, **moved):
        at = dict(own)
        for axis, step in moved.items():
            at[axis] = (own[axis] + step) % RING
        return {"sp": at["z"] * 8 + at["y"] * 2 + (c if c_ is None else c_), "tp": at["x"]}

    partner = device(c_=1 - c)
    other = {"sp": (sp + 31 + 2 * c) % 32, "tp": x}
    near = [device(**{axis: step}) for axis in "xyz" for step in (1, 3, 2)]

    barrier = pltpu.get_barrier_semaphore()
    peers = near + [partner, other]
    for peer in peers:
        pl.semaphore_signal(barrier, inc=1, device_id=peer, device_id_type=MESH)

    def wsel(kind, layer, **at):
        return W.at[(kind, layer) + tuple(at.get(a, own[a]) for a in "xzy") + (c,)]

    locals_ = [
        pltpu.make_async_copy(src, dst, local_sems.at[i])
        for i, (src, dst) in enumerate(
            [(ref.at[l], wsel(k, l)) for l in range(LAYERS) for k, ref in enumerate((val_in, gate_in, out_in))]
            + [
                (tok_in, tok),
                (taps_in.at[pl.ds((HALF - 1) * c, HALF)], own_taps),
                (tok_in.at[x], S.at[x, pl.ds(BLOCK, BLOCK)]),
                (taps_in.at[pl.ds((HALF - 1) * c, HALF)], taps.at[c, x]),
                (gain_in, gain),
                (bias_in, chan.at[0, x]),
                (lng_in, chan.at[1, x]),
                (lns_in, chan.at[2, x]),
            ]
        )
    ]
    for copy in locals_:
        copy.start()
    for copy in locals_:
        copy.wait()
    pl.semaphore_wait(barrier, len(peers))

    copies = Copies(send_sems, recv_sems)
    held = {}
    STEPS = (1, 3, 2)

    def p1(layer):
        for kind in range(3):
            axis = ORDER[kind][0]
            for step in STEPS:
                part = wsel(kind, layer)
                held["p1", layer, kind, step] = copies.start(part, part, device(**{axis: step}))

    def p2_first(layer):
        for kind in range(3):
            for step in STEPS:
                held["p1", layer, kind, step].wait_recv()
            a, b, _ = ORDER[kind]
            part = wsel(kind, layer, **{a: pl.ds(0, 4)})
            for step in (1, 3):
                held["p2", layer, kind, step] = copies.start(part, part, device(**{b: step}))

    def p2_second(layer):
        for kind in range(3):
            a, b, _ = ORDER[kind]
            for half, step in ((0, 1), (2, 3)):
                held["p2", layer, kind, step].wait_recv()
                part = wsel(kind, layer, **{a: pl.ds(half, 2), b: (own[b] + 4 - step) % 4})
                held["p2f", layer, kind, step] = copies.start(part, part, device(**{b: step}))

    def across(layer, kind, at):
        a, b, d = ORDER[kind]
        part = wsel(kind, layer, **{a: pl.ds(0, 4), b: pl.ds(0, 4), d: at})
        held["d2d", layer].append(copies.start(part, part, partner))

    def p3_first(layer):
        held["d2d", layer] = []
        for kind in range(3):
            a, b, d = ORDER[kind]
            for step in (1, 3):
                held["p2f", layer, kind, step].wait_recv()
            part = wsel(kind, layer, **{a: pl.ds(0, 4), b: pl.ds(0, 4)})
            for step in (1, 3):
                held["p3", layer, kind, step] = copies.start(part, part, device(**{d: step}))
            across(layer, kind, own[d])

    def p3_second(layer):
        for kind in range(3):
            a, b, d = ORDER[kind]
            for half, step in ((0, 1), (2, 3)):
                held["p3", layer, kind, step].wait_recv()
                at = (own[d] + 4 - step) % 4
                part = wsel(kind, layer, **{a: pl.ds(half, 2), b: pl.ds(0, 4), d: at})
                held["p3f", layer, kind, step] = copies.start(part, part, device(**{d: step}))
                across(layer, kind, at)

    def p3_last(layer):
        for kind in range(3):
            d = ORDER[kind][2]
            for step in (1, 3):
                held["p3f", layer, kind, step].wait_recv()
            across(layer, kind, (own[d] + 2) % 4)

    def tokens_send():
        for step in STEPS:
            to = (x + step) % 4
            held["tok", step] = copies.start(tok.at[to], S.at[x, pl.ds(BLOCK, BLOCK)], device(x=step))

    def halo_send():
        for step in STEPS:
            held["tok", step].wait_recv()
        block = S.at[:, pl.ds(BLOCK, BLOCK)]
        held["halo"] = [
            copies.start(block, S.at[:, pl.ds(pl.multiple_of(row, BLOCK), BLOCK)], to)
            for row, to in ((2 * BLOCK * c, partner), (2 * BLOCK * (1 - c), other))
        ]

    def params_send():
        held["par"], held["tap"] = [], []
        for step in STEPS:
            held["tap"].append(copies.start(own_taps, taps.at[c, x], device(x=step)))
            for ref, i in ((bias_in, 0), (lng_in, 1), (lns_in, 2)):
                held["par"].append(copies.start(ref, chan.at[i, x], device(x=step)))

    def params_across():
        for copy in held["tap"]:
            copy.wait_recv()
        held["par"].append(copies.start(taps.at[c], taps.at[c], partner))

    row_at = lax.broadcasted_iota(jnp.int32, (3 * BLOCK, CHANS), 0) + (sp * BLOCK - BLOCK)
    inside = jnp.logical_and(row_at >= 0, row_at < 32 * BLOCK)

    def compute(layer):
        r0, rows = HALO * layer, 3 * BLOCK - 2 * HALO * layer
        o0, outs = r0 + HALO, rows - 2 * HALO
        for copy in held["d2d", layer]:
            copy.wait_recv()

        wide = [S[f, r0 : r0 + rows].astype(jnp.float32) for f in range(4)]
        square = wide[0] * wide[0] + wide[1] * wide[1] + wide[2] * wide[2] + wide[3] * wide[3]
        scale = lax.rsqrt(jnp.sum(square, axis=-1, keepdims=True) * (1.0 / (4 * FEATS)) + EPS)
        for f in range(4):
            g = gain[layer : layer + 1, f * FEATS : (f + 1) * FEATS]
            nbuf[r0 : r0 + rows, f * FEATS : (f + 1) * FEATS] = (wide[f] * scale * g).astype(jnp.bfloat16)

        def channel_block(b, carry):
            lhs = nbuf[r0 : r0 + rows]
            rhs = jnp.concatenate(
                [W[k, layer, b].reshape(4 * FEATS, CHANS) for k in (0, 1)], axis=1
            )
            both = jnp.dot(lhs, rhs, preferred_element_type=jnp.float32)
            gated = (both[:, :CHANS] * jax.nn.sigmoid(both[:, CHANS:])).astype(jnp.bfloat16)
            gated = jnp.where(inside[r0 : r0 + rows], gated.astype(jnp.float32), 0.0)
            gbuf[b, r0 : r0 + rows] = gated
            return carry

        lax.fori_loop(0, 4, channel_block, 0)

        def conv_block(b, carry):
            total = jnp.broadcast_to(chan[0, b, layer : layer + 1], (outs, CHANS))
            for k in range(TAPS):
                if k < HALF:
                    t = taps[0, b, k, layer : layer + 1]
                else:
                    t = taps[1, b, k - HALF + 1, layer : layer + 1]
                total = total + gbuf[b, o0 - 15 + k : o0 - 15 + k + outs] * t
            cbuf[b, :outs] = total
            return carry

        lax.fori_loop(0, 4, conv_block, 0)

        conv = [cbuf[b, :outs] for b in range(4)]
        mean = jnp.sum(conv[0] + conv[1] + conv[2] + conv[3], axis=-1, keepdims=True) * (1.0 / 512)
        cent = [v - mean for v in conv]
        square = cent[0] * cent[0] + cent[1] * cent[1] + cent[2] * cent[2] + cent[3] * cent[3]
        scale = lax.rsqrt(jnp.sum(square, axis=-1, keepdims=True) * (1.0 / 512) + EPS)
        for b in range(4):
            n = cent[b] * scale * chan[1, b, layer : layer + 1] + chan[2, b, layer : layer + 1]
            abuf[:outs, b * CHANS : (b + 1) * CHANS] = (n * jax.nn.sigmoid(n)).astype(jnp.bfloat16)

        def out_block(f):
            rhs = jnp.concatenate(
                [W[2, layer, b, f].reshape(FEATS, CHANS) for b in range(4)], axis=1
            )
            branch = lax.dot_general(
                abuf[:outs], rhs, (((1,), (1,)), ((), ())), preferred_element_type=jnp.float32
            )
            return (S[f, o0 : o0 + outs].astype(jnp.float32) + branch).astype(jnp.bfloat16)

        if layer < LAYERS - 1:

            def update(f, carry):
                S[f, o0 : o0 + outs] = out_block(f)
                return carry

            lax.fori_loop(0, 4, update, 0)
        else:
            held["out"] = []
            waiting = []
            for step in (2, 1, 3, 0):
                to = (x + step) % 4
                value = out_block(to)
                if step:
                    obuf[step - 1] = value
                else:
                    out_ref[x] = value
                for s in waiting:
                    held["out"].append(copies.start(obuf.at[s - 1], out_ref.at[x], device(x=s)))
                waiting = [step] if step else []

    p1(0)
    tokens_send()
    p1(1)
    p2_first(0)
    p1(2)
    p1(3)
    p2_second(0)
    p2_first(1)
    params_send()
    halo_send()
    p3_first(0)
    p2_second(1)
    p2_first(2)
    p2_first(3)
    p3_first(1)
    p3_second(0)
    p2_second(2)
    p2_second(3)
    params_across()
    p3_first(2)
    p3_last(0)
    for copy in held["halo"] + held["par"]:
        copy.wait_recv()
    for copy in held["halo"]:
        copy.wait_send()
    compute(0)
    p3_second(1)
    p3_first(3)
    p3_last(1)
    compute(1)
    p3_second(2)
    p3_last(2)
    p3_second(3)
    compute(2)
    p3_last(3)
    compute(3)
    for copy in held["out"]:
        copy.wait_recv()
    for copy in copies.all:
        if all(copy is not done for done in held["halo"]):
            copy.wait_send()


def shards(tokens, norm_gain, val_weight, gate_weight, conv_taps, conv_bias, ln_gain, ln_shift, out_weight):
    copies = 320
    return pl.pallas_call(
        kernel,
        out_shape=jax.ShapeDtypeStruct(tokens.shape, jnp.bfloat16),
        in_specs=[pl.BlockSpec(memory_space=pl.ANY)] * 5
        + [pl.BlockSpec(memory_space=pltpu.VMEM)] * 3
        + [pl.BlockSpec(memory_space=pl.ANY)],
        out_specs=pl.BlockSpec(memory_space=pltpu.VMEM),
        scratch_shapes=[
            pltpu.VMEM((3, LAYERS, 4, 4, 4, 2, SHARD, CHANS), jnp.bfloat16),
            pltpu.VMEM((4, 3 * BLOCK, FEATS), jnp.bfloat16),
            pltpu.VMEM((2, 4, HALF, LAYERS, CHANS), jnp.float32),
            pltpu.VMEM((3, 4, LAYERS, CHANS), jnp.float32),
            pltpu.VMEM((LAYERS, 4 * FEATS), jnp.float32),
            pltpu.VMEM((4, 3 * BLOCK, CHANS), jnp.float32),
            pltpu.VMEM((4, 3 * BLOCK, CHANS), jnp.float32),
            pltpu.VMEM((3 * BLOCK, 4 * FEATS), jnp.bfloat16),
            pltpu.VMEM((3 * BLOCK, 4 * CHANS), jnp.bfloat16),
            pltpu.VMEM((4, BLOCK, FEATS), jnp.bfloat16),
            pltpu.VMEM((HALF, LAYERS, CHANS), jnp.float32),
            pltpu.VMEM((3, BLOCK, FEATS), jnp.bfloat16),
            pltpu.SemaphoreType.DMA((20,)),
            pltpu.SemaphoreType.DMA((copies,)),
            pltpu.SemaphoreType.DMA((copies,)),
        ],
        compiler_params=pltpu.CompilerParams(
            collective_id=0, has_side_effects=True, vmem_limit_bytes=40 * 1024 * 1024
        ),
    )(
        tokens,
        norm_gain,
        val_weight,
        gate_weight,
        jnp.transpose(conv_taps, (1, 0, 2)),
        conv_bias,
        ln_gain,
        ln_shift,
        jnp.transpose(out_weight, (0, 2, 1)),
    )


def solution(mesh):
    return jax.shard_map(
        shards,
        mesh=mesh,
        in_specs=(
            P(None, "sp", "tp"),
            P(),
            P(None, "sp", "tp"),
            P(None, "sp", "tp"),
            P(None, None, "tp"),
            P(None, "tp"),
            P(None, "tp"),
            P(None, "tp"),
            P(None, "tp", "sp"),
        ),
        out_specs=P(None, "sp", "tp"),
        check_vma=False,
    )
```
